512 devices in a mesh: ep: 32 (over z, core), tp: 16 (over y, x).
Axes of the slice: x: 4, y: 4, z: 16, core: 2. Of those that a mesh axis runs over, the one named last changes fastest.
Arguments:
- reception_vectors: bfloat16 [4096, 2048], P('ep', 'tp'), may hold values from -6 to 6
- lookup_vectors: bfloat16 [4096, 2048], P('ep', 'tp'), may hold values from -0.75 to 0.75
- payload_vectors: bfloat16 [4096, 2048], P('ep', 'tp'), may hold values from -6 to 6
- fix_strength_signal: bfloat16 [4096, 2048], P('ep', 'tp'), may hold values from -5 to 5
- fade_signal_term: bfloat16 [4096, 2048], P('ep', 'tp'), may hold values from -8 to 8
- state_erasure: bfloat16 [4096, 2048], P('ep', 'tp'), may hold values from 0 to 1
- feature_speed_pairs: float32 [2, 2048], P(None, 'tp'), as said below
- subspace_scale_vector: float32 [2048], P('tp'), may hold values from 0.1 to 1.9
- subspace_merge_matrix: bfloat16 [2048, 4096], P(None, 'tp'), may hold values from -0.125 to 0.125
- specialist_entry_vectors: bfloat16 [2048, 4096], P('ep'), may hold values from -6 to 6
- specialist_entry_scale: float32 [4096], replicated, may hold values from 0.1 to 1.9
- specialist_picks: int32 [2048, 2], P('ep'), may hold values from 0 to 31, as said below
- dispatch_replica_share: float32 [2048, 2], P('ep'), may hold values from 0.2 to 1
- specialist_valve_matrix: bfloat16 [32, 4096, 2048], P('ep', None, 'tp'), may hold values from -0.09375 to 0.09375
- specialist_raising_matrix: bfloat16 [32, 4096, 2048], P('ep', None, 'tp'), may hold values from -0.09375 to 0.09375
- specialist_lowering_matrix: bfloat16 [32, 2048, 4096], P('ep', None, 'tp'), may hold values from -0.125 to 0.125
Outputs:
- sequence_blend_result: bfloat16 [4096, 4096], P('ep', 'tp')
- expert_out: bfloat16 [2048, 4096], P('ep', 'tp')
The draws below stay inside these ranges and needn't reach their ends.
Inputs may be any that keep to these rules, and one draw needn't show every extreme that they name: `specialist_picks`: the two experts of a row differ and lie in one group, experts g * 8 to g * 8 + 7 for some g. Among the rows of one device (aligned blocks of 64 rows) no expert is named more than 6 times, and some expert exactly 6 times. `feature_speed_pairs`: Finite.
All inputs are finite; a program needn't handle non-finite values.
Results may differ from the reference program's by a relative error of at most 0.0071.
Values may be sent and summed in bfloat16 or wider, within the bound.
A program may use at most 64 MiB of HBM per device.

```python
import math
import jax
import jax.numpy as jnp
from jax import lax

D = 4096
HEAD = 64
WIDTH = 2048
FF = 2048
GROUPS = 4
TOPK = 2
EXPERTS = 32
SPAN = 128
SEQ_A = 4096
TB = 64
TOK_B = 2048
BUSIEST = 24
CAP = 6
N_EP = 32


def draw_feature_speed_pairs(key, part):
    head_count = WIDTH // HEAD
    first, second, third = jax.random.split(key, 3)
    slow_heads = jax.random.uniform(first, (head_count,), jnp.float32) < 0.5
    slow_decay = math.log(0.15 / SEQ_A)
    slow_chan = jnp.repeat(slow_heads, HEAD)
    decay_row = jnp.where(slow_chan, slow_decay, math.log(1.0 / 80.0))
    decay_row = decay_row + jax.random.uniform(second, (WIDTH,), jnp.float32, -0.35, 0.35)
    learn_row = jnp.where(slow_chan, math.log(0.25 * HEAD / SEQ_A), -1.0)
    learn_row = learn_row + jax.random.uniform(third, (WIDTH,), jnp.float32, -0.5, 0.5)
    return jnp.stack([decay_row, learn_row]).astype(jnp.float32)


def draw_fade_signal_term(key, part):
    first, second = jax.random.split(key)
    noise_part = jax.random.normal(first, (SEQ_A, WIDTH), jnp.float32)
    shift_by = jax.random.uniform(second, (N_EP,), jnp.float32, -0.7, 0.7)
    return (noise_part + jnp.repeat(shift_by, SPAN)[:, None]).astype(jnp.bfloat16)


def draw_state_erasure(key, part):
    head_count = WIDTH // HEAD
    first, second = jax.random.split(key)
    where_at = jax.random.randint(first, (head_count, 2), 0, SEQ_A)
    lost_share = jax.random.uniform(second, (head_count, 2), jnp.float32, 0.2, 0.4)
    strength = -jnp.log(1.0 - lost_share)
    hits = (jnp.arange(SEQ_A)[:, None, None] == where_at[None]).astype(jnp.float32) * strength[None]
    per_head = jnp.sum(hits, axis=2)
    return jnp.repeat(per_head, HEAD, axis=1).astype(jnp.bfloat16)


def permute_block(subkey):
    return jax.random.permutation(subkey, TB)


def draw_specialist_picks(key, part):
    blocks = TOK_B // TB
    per_group = EXPERTS // GROUPS
    remaining = TB - BUSIEST
    subkeys = jax.random.split(key, 7)
    top_group = jax.random.randint(subkeys[0], (blocks,), 0, GROUPS)
    group_iota = jnp.arange(GROUPS, dtype=jnp.int32)
    scores = jax.random.randint(subkeys[1], (blocks, GROUPS), 1, 1 << 20) * GROUPS + group_iota[None, :]
    scores = jnp.where(group_iota[None, :] == top_group[:, None], 0, scores)
    group_order = jnp.argsort(scores, axis=1).astype(jnp.int32)
    second_size = jax.random.randint(subkeys[2], (blocks,), max(0, remaining - 2 * BUSIEST), min(BUSIEST, remaining) + 1)
    third_size = jax.random.randint(subkeys[3], (blocks,), jnp.maximum(0, remaining - second_size - BUSIEST), jnp.minimum(BUSIEST, remaining - second_size) + 1)
    bounds = jnp.stack([jnp.zeros((blocks,), jnp.int32), jnp.full((blocks,), BUSIEST, jnp.int32), BUSIEST + second_size, BUSIEST + second_size + third_size], axis=1).astype(jnp.int32)
    position = jnp.arange(TB, dtype=jnp.int32)
    which = (position[None, :] >= bounds[:, 1:2]).astype(jnp.int32) + (position[None, :] >= bounds[:, 2:3]).astype(jnp.int32) + (position[None, :] >= bounds[:, 3:4]).astype(jnp.int32)
    group_id = jnp.take_along_axis(group_order, which, axis=1)
    start_of = jnp.take_along_axis(bounds, which, axis=1)
    rank_in = position[None, :] - start_of
    rotate = jax.random.randint(subkeys[4], (blocks, GROUPS), 0, per_group)
    step_off = jax.random.randint(subkeys[5], (blocks, GROUPS), 1, per_group)
    rot_row = jnp.take_along_axis(rotate, group_id, axis=1)
    off_row = jnp.take_along_axis(step_off, group_id, axis=1)
    first_e = group_id * per_group + (rank_in + rot_row) % per_group
    second_e = group_id * per_group + (rank_in + rot_row + off_row) % per_group
    paired = jnp.stack([first_e, second_e], axis=2)
    shuffle = jax.vmap(permute_block)(jax.random.split(subkeys[6], blocks))
    paired = jnp.take_along_axis(paired, shuffle[:, :, None], axis=1)
    return paired.reshape(TOK_B, 2).astype(jnp.int32)


def level_of(own_key, dims, pieces, low, high):
    level, own = 1.0, jax.random.fold_in(own_key, 6)
    for dim, blocks in pieces:
        draws = jnp.exp(jax.random.uniform(jax.random.fold_in(own, dim), (blocks,), jnp.float32, low / len(pieces), high / len(pieces)))
        level = level * jnp.repeat(draws, dims[dim] // blocks).reshape([-1 if axis == dim else 1 for axis in range(len(dims))])
    return level


def scatter_about(rng, dims, width, reach, shards=(), kind=jnp.bfloat16):
    loudness = level_of(rng, dims, shards, -0.22, 0.18) if shards else 1.0
    values = jax.random.normal(rng, dims, jnp.float32) * width * loudness
    return jnp.minimum(jnp.maximum(values, -reach), reach).astype(kind)


def setup_inputs(seed: int = 0) -> dict:
    seeds = jax.random.split(jax.random.key(seed), 17)
    reception_vectors = scatter_about(seeds[0], (SEQ_A, WIDTH), 1.0, 6.0, ((0, 32), (1, 16)))
    lookup_vectors = scatter_about(seeds[1], (SEQ_A, WIDTH), 0.125, 0.75, ((0, 32), (1, 16)))
    payload_vectors = scatter_about(seeds[2], (SEQ_A, WIDTH), 1.0, 6.0, ((0, 32), (1, 16)))
    fix_strength_signal = scatter_about(seeds[3], (SEQ_A, WIDTH), 1.0, 5.0, ((0, 32), (1, 16)))
    fade_signal_term = draw_fade_signal_term(jax.random.fold_in(seeds[16], 71), 0)
    state_erasure = draw_state_erasure(jax.random.fold_in(seeds[16], 71), 0)
    feature_speed_pairs = draw_feature_speed_pairs(jax.random.fold_in(seeds[16], 71), 0)
    subspace_scale_vector = jnp.clip(1.0 + 0.18 * jax.random.normal(seeds[7], (WIDTH,), jnp.float32), 0.1, 1.9)
    subspace_merge_matrix = scatter_about(seeds[8], (WIDTH, D), WIDTH ** -0.5, 0.125, ((1, 16),))
    specialist_entry_vectors = scatter_about(seeds[9], (TOK_B, D), 1.0, 6.0, ((0, 32),))
    specialist_entry_scale = jnp.clip(1.0 + 0.18 * jax.random.normal(seeds[10], (D,), jnp.float32), 0.1, 1.9)
    specialist_picks = draw_specialist_picks(jax.random.fold_in(seeds[16], 71), 0)
    dispatch_replica_share = jnp.clip(0.2 + 0.8 * jax.random.uniform(seeds[12], (TOK_B, TOPK), jnp.float32) ** level_of(seeds[12], (TOK_B, TOPK), ((0, 32),), -0.2, 0.2), 0.2, 1.0)
    specialist_valve_matrix = scatter_about(seeds[13], (EXPERTS, D, FF), D ** -0.5, 0.09375, ((0, 32), (2, 16)))
    specialist_raising_matrix = scatter_about(seeds[14], (EXPERTS, D, FF), D ** -0.5, 0.09375, ((0, 32), (2, 16)))
    specialist_lowering_matrix = scatter_about(seeds[15], (EXPERTS, FF, D), FF ** -0.5, 0.125, ((0, 32), (2, 16)))
    return dict(reception_vectors=reception_vectors, lookup_vectors=lookup_vectors, payload_vectors=payload_vectors, fix_strength_signal=fix_strength_signal, fade_signal_term=fade_signal_term, state_erasure=state_erasure, feature_speed_pairs=feature_speed_pairs, subspace_scale_vector=subspace_scale_vector, subspace_merge_matrix=subspace_merge_matrix, specialist_entry_vectors=specialist_entry_vectors, specialist_entry_scale=specialist_entry_scale, specialist_picks=specialist_picks, dispatch_replica_share=dispatch_replica_share, specialist_valve_matrix=specialist_valve_matrix, specialist_raising_matrix=specialist_raising_matrix, specialist_lowering_matrix=specialist_lowering_matrix)


highest = lax.Precision.HIGHEST

def blend_sequence(reception_vectors, lookup_vectors, payload_vectors, fix_strength_signal, fade_signal_term, state_erasure, feature_speed_pairs, subspace_scale_vector, subspace_merge_matrix):
    seq_len, channels = reception_vectors.shape
    head_count = channels // HEAD
    fade_speed_exponent = jnp.exp(-jnp.exp(feature_speed_pairs[0] + fade_signal_term.astype(jnp.float32)) - state_erasure.astype(jnp.float32))
    learn_rate = jax.nn.sigmoid(fix_strength_signal.astype(jnp.float32) + feature_speed_pairs[1])

    def split_heads(array):
        return array.astype(jnp.float32).reshape(seq_len, head_count, HEAD)
    key_heads = split_heads(lookup_vectors)
    key_unit = key_heads * lax.rsqrt(lax.optimization_barrier(jnp.sum(key_heads * key_heads, axis=-1, keepdims=True)) + 1e-06)

    def advance(state_mat, inputs):
        step_recept, step_decay, step_key, step_value, step_unit, step_learn = inputs
        state_hit = jnp.einsum('hvk,hk->hv', state_mat, step_unit, precision=highest)
        state_mat = state_mat * step_decay[:, None, :] - state_hit[:, :, None] * (step_unit * step_learn)[:, None, :] + step_value[:, :, None] * step_key[:, None, :]
        return (state_mat, jnp.einsum('hvk,hk->hv', state_mat, step_recept, precision=highest))
    initial = jnp.zeros((head_count, HEAD, HEAD), jnp.float32)
    final_state, outputs = lax.scan(advance, initial, (split_heads(reception_vectors), fade_speed_exponent.reshape(seq_len, head_count, HEAD), key_heads, split_heads(payload_vectors), key_unit, learn_rate.reshape(seq_len, head_count, HEAD)))
    head_mean = lax.optimization_barrier(jnp.mean(outputs, axis=-1, keepdims=True))
    centred = outputs - head_mean
    head_var = lax.optimization_barrier(jnp.mean(centred * centred, axis=-1, keepdims=True))
    scaled = centred * lax.rsqrt(head_var + 0.00064) * subspace_scale_vector.reshape(head_count, HEAD)
    mixed_rows = scaled.reshape(seq_len, channels).astype(jnp.bfloat16)
    return jnp.dot(mixed_rows, subspace_merge_matrix, preferred_element_type=jnp.float32).astype(jnp.bfloat16)

def expert_layer(specialist_entry_vectors, specialist_entry_scale, specialist_picks, dispatch_replica_share, specialist_valve_matrix, specialist_raising_matrix, specialist_lowering_matrix):
    widened = specialist_entry_vectors.astype(jnp.float32)
    normed = (widened * lax.rsqrt(lax.optimization_barrier(jnp.mean(widened * widened, axis=-1, keepdims=True)) + 1e-06) * specialist_entry_scale).astype(jnp.bfloat16)
    flat_ids = specialist_picks.reshape(-1).astype(jnp.int32)
    flat_weight = dispatch_replica_share.reshape(-1)
    token_of = (jnp.arange(flat_ids.shape[0], dtype=jnp.int32) // TOPK).astype(jnp.int32)
    max_rows = N_EP * CAP

    def run_expert(running, expert):
        order_idx = jnp.argsort((flat_ids != expert).astype(jnp.int32), stable=True)[:max_rows]
        chosen = token_of[order_idx]
        live_weight = jnp.where(flat_ids[order_idx] == expert, flat_weight[order_idx], 0.0)
        rows_in = normed[chosen]
        gate_part = jnp.dot(rows_in, specialist_valve_matrix[expert], preferred_element_type=jnp.float32)
        up_part = jnp.dot(rows_in, specialist_raising_matrix[expert], preferred_element_type=jnp.float32)
        hidden = (jax.nn.silu(gate_part) * up_part).astype(jnp.bfloat16)
        result = jnp.dot(hidden, specialist_lowering_matrix[expert], preferred_element_type=jnp.float32).astype(jnp.bfloat16)
        running = running.at[chosen].add(result.astype(jnp.float32) * live_weight[:, None])
        return (running, None)
    running, unused = lax.scan(run_expert, jnp.zeros(specialist_entry_vectors.shape, jnp.float32), jnp.arange(EXPERTS, dtype=jnp.int32))
    return running.astype(jnp.bfloat16)

def reference(reception_vectors, lookup_vectors, payload_vectors, fix_strength_signal, fade_signal_term, state_erasure, feature_speed_pairs, subspace_scale_vector, subspace_merge_matrix, specialist_entry_vectors, specialist_entry_scale, specialist_picks, dispatch_replica_share, specialist_valve_matrix, specialist_raising_matrix, specialist_lowering_matrix):
    sequence_blend_result = blend_sequence(reception_vectors, lookup_vectors, payload_vectors, fix_strength_signal, fade_signal_term, state_erasure, feature_speed_pairs, subspace_scale_vector, subspace_merge_matrix)
    expert_out = expert_layer(specialist_entry_vectors, specialist_entry_scale, specialist_picks, dispatch_replica_share, specialist_valve_matrix, specialist_raising_matrix, specialist_lowering_matrix)
    return (sequence_blend_result, expert_out)
```

```python
import jax
import jax.numpy as jnp
from jax import lax
from jax.experimental import pallas as pl
from jax.experimental.pallas import tpu as pltpu
from jax.sharding import PartitionSpec as P

HEAD = 64
SLOTS = 8
CAP = 6
F32, BF16 = jnp.float32, jnp.bfloat16
MESH = pl.DeviceIdType.MESH


def dot(a, b, ca, cb):
    return lax.dot_general(a, b, (((ca,), (cb,)), ((), ())), preferred_element_type=F32)


def split(a):
    high = a.astype(BF16)
    return high, (a - high.astype(F32)).astype(BF16)


def dot3(a, b, ca=1, cb=0):
    a_hi, a_lo = split(a)
    b_hi, b_lo = split(b)
    return dot(a_hi, b_hi, ca, cb) + (dot(a_hi, b_lo, ca, cb) + dot(a_lo, b_hi, ca, cb))


def sums_of(choice, parts):
    return sum(dot(choice, part, 1, 0) for part in parts)


def chosen(mask):
    return mask.astype(F32).astype(BF16)


def iota(shape, axis):
    return lax.broadcasted_iota(jnp.int32, shape, axis)


def per_head(array):
    first = iota(array.shape, 1) < HEAD
    low = jnp.sum(jnp.where(first, array, 0.0), axis=1, keepdims=True)
    high = jnp.sum(jnp.where(first, 0.0, array), axis=1, keepdims=True)
    return low, high


def by_head(low, high, shape):
    return jnp.where(iota(shape, 1) < HEAD, low, high)


def pair_matrices(recept, key, value, fix, fade, erase, speeds):
    n, c = key.shape
    recept, key, value = recept.astype(F32), key.astype(F32), value.astype(F32)
    log_decay = -jnp.exp(speeds[0:1] + fade.astype(F32)) - erase.astype(F32)
    log_decay = jnp.maximum(log_decay, -100.0)
    learn = 1.0 / (1.0 + jnp.exp(-(fix.astype(F32) + speeds[1:2])))
    first = iota((n, c), 1) < HEAD
    unit = key * lax.rsqrt(by_head(*per_head(key * key), (n, c)) + 1e-6)
    removal = unit * learn

    part_a = log_decay.astype(BF16)
    rest = log_decay - part_a.astype(F32)
    part_b = rest.astype(BF16)
    part_c = (rest - part_b.astype(F32)).astype(BF16)
    parts = (part_a, part_b, part_c)

    row, col, pos = iota((n, n), 0), iota((n, n), 1), iota((n, c), 0)
    differ = row ^ col

    def both_heads(array):
        return jnp.concatenate([jnp.where(first, array, 0.0), jnp.where(first, 0.0, array)], 0)

    total = jnp.zeros((4 * n, 2 * n), F32)
    size = 1
    while size < n:
        later = (row & size) != 0
        mid = row & ~(size - 1)
        key_rows = chosen(later & (col >= mid) & (col < row))
        read_rows = chosen(later & (col >= mid) & (col <= row))
        end = (row | (size - 1)) + 1
        write_rows = chosen(jnp.logical_not(later) & (col > row) & (col < end))
        is_later = (pos & size) != 0
        key_in = jnp.where(is_later, unit * jnp.exp(sums_of(key_rows, parts)), 0.0)
        read_in = jnp.where(is_later, recept * jnp.exp(sums_of(read_rows, parts)), 0.0)
        fading = jnp.where(is_later, 0.0, jnp.exp(sums_of(write_rows, parts)))
        left = jnp.concatenate([both_heads(key_in), both_heads(read_in)], 0)
        right = jnp.concatenate([removal * fading, key * fading], 0)
        found = dot3(left, right, 1, 1)
        level = (differ >= size) & (differ < 2 * size) & (row > col)
        level = jnp.concatenate([level, level], 1)
        level = jnp.concatenate([level, level, level, level], 0)
        total = jnp.where(level, found, total)
        size *= 2
    return recept, key, value, unit, removal, log_decay, parts, total


def pair_results(recept, key, value, unit, removal, log_decay, parts, total):
    n, c = key.shape
    row, col = iota((n, n), 0), iota((n, n), 1)
    differ = row ^ col
    first = iota((n, c), 1) < HEAD

    def pick_lanes(pair):
        return jnp.where(first, pair[0], pair[1])

    eye = row == col
    own_write = per_head(recept * key)
    own_removal = per_head(recept * removal)
    heads = range(2)
    solve_mat = [total[h * n : (h + 1) * n, :n] for h in heads]
    solve_val = [total[h * n : (h + 1) * n, n:] for h in heads]
    read_rem = [jnp.where(eye, own_removal[h], total[(2 + h) * n : (3 + h) * n, :n]) for h in heads]
    read_val = [jnp.where(eye, own_write[h], total[(2 + h) * n : (3 + h) * n, n:]) for h in heads]

    below = row > col
    inverse = [
        jnp.where(eye, 1.0, jnp.where((differ == 1) & below, -solve_mat[h], 0.0)) for h in heads
    ]
    size = 2
    while size < n:
        level = (differ >= size) & (differ < 2 * size) & below
        inner = [dot3(jnp.where(level, solve_mat[h], 0.0), inverse[h]) for h in heads]
        inverse = [inverse[h] - dot3(inverse[h], inner[h]) for h in heads]
        size *= 2

    before = sums_of(chosen(col < row), parts)
    upto = before + log_decay
    after = sums_of(chosen(col > row), parts)
    key_start = unit * jnp.exp(before)
    read_start = recept * jnp.exp(upto)
    to_end = jnp.exp(after)
    whole = jnp.exp(upto[n - 1 : n])

    hit_val = pick_lanes([dot3(solve_val[h], value) for h in heads])
    both = jnp.concatenate([key_start, hit_val], 1)
    hits = [dot3(inverse[h], both) for h in heads]
    both = jnp.concatenate(
        [pick_lanes([hits[h][:, :c] for h in heads]), pick_lanes([hits[h][:, c:] for h in heads])],
        1,
    )
    taken = [dot3(read_rem[h], both) for h in heads]
    carried = read_start - pick_lanes([taken[h][:, :c] for h in heads])
    own_out = pick_lanes([dot3(read_val[h], value) - taken[h][:, c:] for h in heads])

    removed = dot3(removal * to_end, both, 0, 0)
    written = dot3(key * to_end, value, 0, 0)
    trans = jnp.where(eye, whole, 0.0) - removed[:, :c]
    state = written - removed[:, c:]
    pair = jnp.concatenate(
        [
            jnp.concatenate([trans[:HEAD, :HEAD], state[:HEAD, :HEAD]], 1),
            jnp.concatenate([trans[HEAD:, HEAD:], state[HEAD:, HEAD:]], 1),
        ],
        0,
    )
    return carried, own_out, pair


def compose(earlier, later):
    right = iota(later.shape, 1) >= HEAD
    return dot3(later[:, :HEAD], earlier) + jnp.where(right, later, 0.0)


class Gather:
    def __init__(self, buf, send_sem, recv_sem, place, ny, nx):
        self.buf, self.send_sem, self.recv_sem = buf, send_sem, recv_sem
        self.ep, self.y, self.x = place
        self.ny, self.nx = ny, nx
        self.half = buf.shape[2] // 2

    def block(self, half, phase, step, begin, count):
        rows = pl.ds(half * self.half + begin, count)
        if (half + phase) % 2 == 0:
            at = lax.rem(self.x + step + self.nx, self.nx)
            if phase == 0:
                return self.buf.at[self.y, at, rows]
            return self.buf.at[:, at, rows]
        at = lax.rem(self.y + step + self.ny, self.ny)
        if phase == 0:
            return self.buf.at[at, self.x, rows]
        return self.buf.at[at, :, rows]

    def other(self, half, phase, step):
        if (half + phase) % 2 == 0:
            x, y = lax.rem(self.x + step + self.nx, self.nx), self.y
        else:
            x, y = self.x, lax.rem(self.y + step + self.ny, self.ny)
        return {"ep": self.ep, "tp": y * self.nx + x}

    def sent(self, half, phase, kind):
        part = self.half // 2
        step, begin, count, to = (
            (0, 0, 2 * part, 1),
            (0, 0, 2 * part, -1),
            (-1, 0, part, 1),
            (1, part, part, -1),
        )[kind]
        block = self.block(half, phase, step, begin, count)
        at = (half * 2 + phase) * 4 + kind
        return pltpu.make_async_remote_copy(
            src_ref=block,
            dst_ref=block,
            send_sem=self.send_sem.at[at],
            recv_sem=self.recv_sem.at[at],
            device_id=self.other(half, phase, to),
            device_id_type=MESH,
        )

    def arrived(self, half, phase, kind):
        part = self.half // 2
        step, begin, count = (
            (-1, 0, 2 * part),
            (1, 0, 2 * part),
            (-2, 0, part),
            (2, part, part),
        )[kind]
        block = self.block(half, phase, step, begin, count)
        at = (half * 2 + phase) * 4 + kind
        pltpu.make_async_copy(block, block, self.recv_sem.at[at]).wait()

    def start(self, half, phase):
        self.sent(half, phase, 0).start()
        self.sent(half, phase, 1).start()

    def forward(self, half, phase):
        self.arrived(half, phase, 0)
        self.sent(half, phase, 2).start()
        self.arrived(half, phase, 1)
        self.sent(half, phase, 3).start()

    def finish(self, half, phase):
        self.arrived(half, phase, 2)
        self.arrived(half, phase, 3)

    def drain(self):
        for half in range(2):
            for phase in range(2):
                for kind in range(4):
                    self.sent(half, phase, kind).wait_send()


def wait_for(ref, sem):
    pltpu.make_async_copy(ref, ref, sem).wait()


def kernel(
    n_ep,
    n_y,
    n_x,
    group,
    recept_ref,
    key_ref,
    value_ref,
    fix_ref,
    fade_ref,
    erase_ref,
    speeds_ref,
    gain_ref,
    merge_hbm,
    rows_ref,
    scale_ref,
    picks_ref,
    share_ref,
    gate_hbm,
    up_hbm,
    down_hbm,
    blend_out,
    expert_out,
    merge_ref,
    gate_up_ref,
    down_ref,
    send_buf,
    recv_buf,
    rows_all,
    hidden_all,
    back_buf,
    ret_buf,
    mixed_all,
    pair_buf,
    pair_in,
    chip_pairs,
    group_pairs,
    state_out,
    state_in,
    load_sem,
    ep_send,
    ep_recv,
    x_send,
    x_recv,
    h_send,
    h_recv,
    m_send,
    m_recv,
    scan_send,
    scan_recv,
):
    ep, tp = lax.axis_index("ep"), lax.axis_index("tp")
    core, z = lax.rem(ep, 2), ep // 2
    y, x = tp // n_x, lax.rem(tp, n_x)
    place = lax.rem(z, group)
    n_group = n_ep // 2 // group
    mine = z // group
    partner = ep + 1 - 2 * core
    n, c = key_ref.shape
    n_rows = rows_ref.shape[0]
    lanes = send_buf.shape[2]
    slots = n_ep * SLOTS
    depth = gate_hbm.shape[1]

    loads = [
        pltpu.make_async_copy(gate_hbm, gate_up_ref.at[:, pl.ds(0, depth)], load_sem.at[0]),
        pltpu.make_async_copy(up_hbm, gate_up_ref.at[:, pl.ds(depth, depth)], load_sem.at[1]),
        pltpu.make_async_copy(down_hbm, down_ref, load_sem.at[2]),
        pltpu.make_async_copy(merge_hbm, merge_ref, load_sem.at[3]),
    ]
    for load in loads:
        load.start()

    barrier = pltpu.get_barrier_semaphore()

    def greet(step, carry):
        pl.semaphore_signal(
            barrier,
            inc=1,
            device_id={"ep": lax.rem(ep + step, n_ep), "tp": tp},
            device_id_type=MESH,
        )
        return carry

    lax.fori_loop(1, n_ep, greet, 0)
    for step in (1, -1):
        for other in (
            y * n_x + lax.rem(x + step + n_x, n_x),
            lax.rem(y + step + n_y, n_y) * n_x + x,
        ):
            pl.semaphore_signal(
                barrier, inc=1, device_id={"ep": ep, "tp": other}, device_id_type=MESH
            )

    widened = rows_ref[...].astype(F32)
    strength = lax.rsqrt(jnp.mean(widened * widened, axis=1, keepdims=True) + 1e-6)
    own = pl.ds(pl.multiple_of(tp * lanes, 128), lanes)
    normed = (rows_ref[:, own].astype(F32) * strength * scale_ref[:, own]).astype(BF16)
    slot = iota((n_rows, slots), 1)
    expert = slot // SLOTS
    named = [picks_ref[:, k : k + 1] == expert for k in range(2)]
    either = named[0] | named[1]
    earlier = chosen(iota((n_rows, n_rows), 1) < iota((n_rows, n_rows), 0))
    rank = dot(earlier, chosen(either), 1, 0)
    taken = either & (rank == lax.rem(slot, SLOTS).astype(F32))
    weight = jnp.where(taken & named[0], share_ref[:, 0:1], 0.0) + jnp.where(
        taken & named[1], share_ref[:, 1:2], 0.0
    )
    send_buf[...] = dot(chosen(taken), normed, 0, 0).reshape(n_ep, SLOTS, lanes).astype(BF16)

    matrices = pair_matrices(
        recept_ref[...],
        key_ref[...],
        value_ref[...],
        fix_ref[...],
        fade_ref[...],
        erase_ref[...],
        speeds_ref[...],
    )

    pl.semaphore_wait(barrier, n_ep - 1 + 4)

    def ep_copy(src, dst, step, at):
        other = lax.rem(ep + step, n_ep)
        return pltpu.make_async_remote_copy(
            src_ref=src.at[other],
            dst_ref=dst.at[ep],
            send_sem=ep_send.at[at],
            recv_sem=ep_recv.at[at],
            device_id={"ep": other, "tp": tp},
            device_id_type=MESH,
        )

    def ep_exchange(src, dst, at):
        def send(step, carry):
            ep_copy(src, dst, step, at).start()
            return carry

        lax.fori_loop(1, n_ep, send, 0)
        dst[ep] = src[ep]

    ep_exchange(send_buf, recv_buf, 0)

    carried, own_out, pair = pair_results(*matrices)
    pair_buf[...] = pair

    def scan_copy(src, dst, device, at):
        return pltpu.make_async_remote_copy(
            src_ref=src,
            dst_ref=dst,
            send_sem=scan_send.at[at],
            recv_sem=scan_recv.at[at],
            device_id={"ep": device, "tp": tp},
            device_id_type=MESH,
        )

    theirs = pair_buf.at[pl.ds(pl.multiple_of(HEAD * (1 - core), HEAD), HEAD)]
    swap = scan_copy(theirs, pair_in, partner, 0)
    swap.start()
    swap.wait_recv()
    own_pair = pair_buf[pl.ds(pl.multiple_of(HEAD * core, HEAD), HEAD), :]
    other_pair = pair_in[...]
    even = core == 0
    pair_0 = jnp.where(even, own_pair, other_pair)
    pair_1 = jnp.where(even, other_pair, own_pair)
    chip_pairs[place] = compose(pair_0, pair_1)
    local = []
    for step in range(1, group):
        at = lax.rem(place + step, group)
        local.append(
            scan_copy(
                chip_pairs.at[place],
                chip_pairs.at[place],
                2 * (mine * group + at) + core,
                step,
            )
        )
        local[-1].start()
    for step in range(1, group):
        at = lax.rem(place - step + group, group)
        wait_for(chip_pairs.at[at], scan_recv.at[step])
    prefix = [chip_pairs[0]]
    for at in range(1, group):
        prefix.append(compose(prefix[-1], chip_pairs[at]))
    ident = jnp.where(iota((HEAD, c), 0) == iota((HEAD, c), 1), 1.0, 0.0)
    inside = ident
    for at in range(group - 1):
        inside = jnp.where(place == at + 1, prefix[at], inside)
    group_pairs[mine] = prefix[-1]

    def group_copy(step):
        return scan_copy(
            group_pairs.at[mine],
            group_pairs.at[mine],
            2 * ((mine + step) * group + place) + core,
            group + step - 1,
        )

    for step in range(1, n_group):

        @pl.when(mine + step < n_group)
        def _(step=step):
            group_copy(step).start()

    wait_for(recv_buf.at[pl.ds(0, n_ep - 1)], ep_recv.at[0])
    packed, spread = iota((n_ep * CAP, slots), 0), iota((n_ep * CAP, slots), 1)
    inner = lax.rem(spread, SLOTS)
    pack = chosen((inner < CAP) & (spread // SLOTS * CAP + inner == packed))
    arrived = recv_buf[...].astype(F32).reshape(slots, lanes).astype(BF16)
    rows_all[y, x] = dot(pack, arrived, 1, 0).astype(BF16)

    spot = (ep, y, x)
    xs = Gather(rows_all, x_send, x_recv, spot, n_y, n_x)
    hs = Gather(hidden_all, h_send, h_recv, spot, n_y, n_x)
    ms = Gather(mixed_all, m_send, m_recv, spot, n_y, n_x)
    both = (0, 1)
    for half in both:
        xs.start(half, 0)
    for half in both:
        xs.forward(half, 0)
    for half in both:
        xs.finish(half, 0)
        xs.start(half, 1)

    for step in range(1, n_group):

        @pl.when(mine >= step)
        def _(step=step):
            wait_for(group_pairs.at[mine - step], scan_recv.at[group + step - 1])

    state = jnp.zeros((HEAD, c), F32)
    for at in range(n_group - 1):
        state = jnp.where(at < mine, compose(state, group_pairs[at]), state)
    state_0 = compose(state, inside)
    state_1 = compose(state_0, pair_0)
    state_out[...] = jnp.where(even, state_1, state_0)
    give = scan_copy(state_out, state_in, partner, group + n_group - 1)
    give.start()
    state_own = jnp.where(even, state_0, state_1)

    for half in both:
        xs.forward(half, 1)

    give.wait_recv()
    state_other = state_in[...]
    state_a = jnp.where(even, state_own, state_other)
    state_b = jnp.where(even, state_other, state_own)
    right = iota((HEAD, c), 1) >= HEAD
    entering = jnp.concatenate(
        [
            jnp.concatenate([state_a[:, HEAD:], jnp.zeros((HEAD, HEAD), F32)], 1),
            jnp.where(right, state_b, 0.0),
        ],
        0,
    )
    out = dot3(carried, entering) + own_out
    mean = by_head(*per_head(out), (n, c)) * (1.0 / HEAD)
    centred = out - mean
    spread_of = by_head(*per_head(centred * centred), (n, c)) * (1.0 / HEAD)
    mixed = centred * lax.rsqrt(spread_of + 0.00064) * gain_ref[...]
    mixed_all[y, x] = mixed.astype(BF16)
    for half in both:
        ms.start(half, 0)

    for half in both:
        xs.finish(half, 1)
    for load in loads[:2]:
        load.wait()

    total = jnp.zeros((n_ep * CAP, 2 * depth), F32)
    for j in range(n_y * n_x):
        total = total + dot(
            rows_all[j // n_x, j % n_x], gate_up_ref[j * lanes : (j + 1) * lanes, :], 1, 0
        )
    gated, raised = total[:, :depth], total[:, depth:]
    hidden_all[y, x] = (gated / (1.0 + jnp.exp(-gated)) * raised).astype(BF16)
    for half in both:
        hs.start(half, 0)
    for half in both:
        ms.forward(half, 0)
    for half in both:
        hs.forward(half, 0)
    for half in both:
        hs.finish(half, 0)
        hs.start(half, 1)
    for half in both:
        ms.finish(half, 0)
        ms.start(half, 1)
    for half in both:
        hs.forward(half, 1)
    for half in both:
        ms.forward(half, 1)
    for half in both:
        hs.finish(half, 1)
    loads[2].wait()
    result = jnp.zeros((n_ep * CAP, lanes), F32)
    for j in range(n_y * n_x):
        result = result + dot(
            hidden_all[j // n_x, j % n_x], down_ref[j * depth : (j + 1) * depth, :], 1, 0
        )
    back_buf[...] = dot(pack, result.astype(BF16), 0, 0).reshape(n_ep, SLOTS, lanes).astype(BF16)
    ep_exchange(back_buf, ret_buf, 1)

    for half in both:
        ms.finish(half, 1)
    loads[3].wait()
    blend = jnp.zeros(blend_out.shape, F32)
    for j in range(n_y * n_x):
        blend = blend + dot(mixed_all[j // n_x, j % n_x], merge_ref[j * c : (j + 1) * c, :], 1, 0)
    blend_out[...] = blend.astype(BF16)

    for gather in (xs, hs, ms):
        gather.drain()
    swap.wait_send()
    give.wait_send()
    for copy in local:
        copy.wait_send()
    for step in range(1, n_group):

        @pl.when(mine + step < n_group)
        def _(step=step):
            group_copy(step).wait_send()

    wait_for(send_buf.at[pl.ds(0, n_ep - 1)], ep_send.at[0])
    wait_for(ret_buf.at[pl.ds(0, n_ep - 1)], ep_recv.at[1])
    returned = ret_buf[...].astype(F32).reshape(slots, lanes).astype(BF16)
    w_hi, w_lo = split(weight)
    expert_out[...] = (dot(w_hi, returned, 1, 0) + dot(w_lo, returned, 1, 0)).astype(BF16)
    wait_for(back_buf.at[pl.ds(0, n_ep - 1)], ep_send.at[1])


def body(
    n_ep,
    n_y,
    n_x,
    group,
    recept,
    key,
    value,
    fix,
    fade,
    erase,
    speeds,
    gain,
    merge,
    rows,
    scale,
    picks,
    share,
    gate,
    up,
    down,
):
    n, c = key.shape
    n_rows, width = rows.shape
    lanes = down.shape[2]
    depth = gate.shape[2]
    slots = n_ep * CAP
    n_group = n_ep // 2 // group
    scans = group + n_group
    vmem, hbm = pl.BlockSpec(memory_space=pltpu.VMEM), pl.BlockSpec(memory_space=pltpu.HBM)
    dma = pltpu.SemaphoreType.DMA
    return pl.pallas_call(
        lambda *refs: kernel(n_ep, n_y, n_x, group, *refs),
        out_shape=(
            jax.ShapeDtypeStruct((n, merge.shape[1]), BF16),
            jax.ShapeDtypeStruct((n_rows, lanes), BF16),
        ),
        in_specs=[vmem] * 8 + [hbm] + [vmem] * 4 + [hbm] * 3,
        out_specs=(vmem, vmem),
        scratch_shapes=[
            pltpu.VMEM(merge.shape, BF16),
            pltpu.VMEM((width, 2 * depth), BF16),
            pltpu.VMEM(down.shape[1:], BF16),
            pltpu.VMEM((n_ep, SLOTS, lanes), BF16),
            pltpu.VMEM((n_ep, SLOTS, lanes), BF16),
            pltpu.VMEM((n_y, n_x, slots, lanes), BF16),
            pltpu.VMEM((n_y, n_x, slots, depth), BF16),
            pltpu.VMEM((n_ep, SLOTS, lanes), BF16),
            pltpu.VMEM((n_ep, SLOTS, lanes), BF16),
            pltpu.VMEM((n_y, n_x, n, c), BF16),
            pltpu.VMEM((n, c), F32),
            pltpu.VMEM((HEAD, c), F32),
            pltpu.VMEM((group, HEAD, c), F32),
            pltpu.VMEM((n_group, HEAD, c), F32),
            pltpu.VMEM((HEAD, c), F32),
            pltpu.VMEM((HEAD, c), F32),
            dma((4,)),
            dma((2,)),
            dma((2,)),
            dma((16,)),
            dma((16,)),
            dma((16,)),
            dma((16,)),
            dma((16,)),
            dma((16,)),
            dma((scans,)),
            dma((scans,)),
        ],
        compiler_params=pltpu.CompilerParams(
            collective_id=0, has_side_effects=True, vmem_limit_bytes=56 << 20
        ),
    )(
        recept,
        key,
        value,
        fix,
        fade,
        erase,
        speeds,
        gain.reshape(1, c),
        merge,
        rows,
        scale.reshape(1, width),
        picks,
        share,
        gate[0],
        up[0],
        down[0],
    )


def solution(mesh):
    n_ep, n_tp = mesh.shape["ep"], mesh.shape["tp"]
    n_x = 4
    group = 4
    placed = (
        *(P("ep", "tp"),) * 6,
        P(None, "tp"),
        P("tp"),
        P(None, "tp"),
        P("ep", None),
        P(),
        P("ep", None),
        P("ep", None),
        *(P("ep", None, "tp"),) * 3,
    )
    return jax.shard_map(
        lambda *args: body(n_ep, n_tp // n_x, n_x, group, *args),
        mesh=mesh,
        in_specs=placed,
        out_specs=(P("ep", "tp"), P("ep", "tp")),
        check_vma=False,
    )
```

```python
import jax
import jax.numpy as jnp
from jax import lax
from jax.experimental import pallas as pl
from jax.experimental.pallas import tpu as pltpu
from jax.sharding import PartitionSpec as P

HEAD = 64
SLOTS = 8
CAP = 6
CHUNKS = 2
F32, BF16 = jnp.float32, jnp.bfloat16
MESH = pl.DeviceIdType.MESH


def dot(a, b, ca, cb):
    return lax.dot_general(a, b, (((ca,), (cb,)), ((), ())), preferred_element_type=F32)


def split(a):
    high = a.astype(BF16)
    return high, (a - high.astype(F32)).astype(BF16)


def dot3(a, b, ca=1, cb=0):
    a_hi, a_lo = split(a)
    b_hi, b_lo = split(b)
    return dot(a_hi, b_hi, ca, cb) + (dot(a_hi, b_lo, ca, cb) + dot(a_lo, b_hi, ca, cb))


def sums_of(choice, parts):
    return sum(dot(choice, part, 1, 0) for part in parts)


def chosen(mask):
    return mask.astype(F32).astype(BF16)


def iota(shape, axis):
    return lax.broadcasted_iota(jnp.int32, shape, axis)


def per_head(array):
    first = iota(array.shape, 1) < HEAD
    low = jnp.sum(jnp.where(first, array, 0.0), axis=1, keepdims=True)
    high = jnp.sum(jnp.where(first, 0.0, array), axis=1, keepdims=True)
    return low, high


def by_head(low, high, shape):
    return jnp.where(iota(shape, 1) < HEAD, low, high)


def pair_matrices(recept, key, value, fix, fade, erase, speeds):
    n, c = key.shape
    recept, key, value = recept.astype(F32), key.astype(F32), value.astype(F32)
    log_decay = -jnp.exp(speeds[0:1] + fade.astype(F32)) - erase.astype(F32)
    log_decay = jnp.maximum(log_decay, -100.0)
    learn = 1.0 / (1.0 + jnp.exp(-(fix.astype(F32) + speeds[1:2])))
    first = iota((n, c), 1) < HEAD
    unit = key * lax.rsqrt(by_head(*per_head(key * key), (n, c)) + 1e-6)
    removal = unit * learn

    part_a = log_decay.astype(BF16)
    rest = log_decay - part_a.astype(F32)
    part_b = rest.astype(BF16)
    part_c = (rest - part_b.astype(F32)).astype(BF16)
    parts = (part_a, part_b, part_c)

    row, col, pos = iota((n, n), 0), iota((n, n), 1), iota((n, c), 0)
    differ = row ^ col

    def both_heads(array):
        return jnp.concatenate([jnp.where(first, array, 0.0), jnp.where(first, 0.0, array)], 0)

    total = jnp.zeros((4 * n, 2 * n), F32)
    size = 1
    while size < n:
        later = (row & size) != 0
        mid = row & ~(size - 1)
        key_rows = chosen(later & (col >= mid) & (col < row))
        read_rows = chosen(later & (col >= mid) & (col <= row))
        end = (row | (size - 1)) + 1
        write_rows = chosen(jnp.logical_not(later) & (col > row) & (col < end))
        is_later = (pos & size) != 0
        key_in = jnp.where(is_later, unit * jnp.exp(sums_of(key_rows, parts)), 0.0)
        read_in = jnp.where(is_later, recept * jnp.exp(sums_of(read_rows, parts)), 0.0)
        fading = jnp.where(is_later, 0.0, jnp.exp(sums_of(write_rows, parts)))
        left = jnp.concatenate([both_heads(key_in), both_heads(read_in)], 0)
        right = jnp.concatenate([removal * fading, key * fading], 0)
        found = dot3(left, right, 1, 1)
        level = (differ >= size) & (differ < 2 * size) & (row > col)
        level = jnp.concatenate([level, level], 1)
        level = jnp.concatenate([level, level, level, level], 0)
        total = jnp.where(level, found, total)
        size *= 2
    return recept, key, value, unit, removal, log_decay, parts, total


def pair_results(recept, key, value, unit, removal, log_decay, parts, total):
    n, c = key.shape
    row, col = iota((n, n), 0), iota((n, n), 1)
    differ = row ^ col
    first = iota((n, c), 1) < HEAD

    def pick_lanes(pair):
        return jnp.where(first, pair[0], pair[1])

    eye = row == col
    own_write = per_head(recept * key)
    own_removal = per_head(recept * removal)
    heads = range(2)
    solve_mat = [total[h * n : (h + 1) * n, :n] for h in heads]
    solve_val = [total[h * n : (h + 1) * n, n:] for h in heads]
    read_rem = [jnp.where(eye, own_removal[h], total[(2 + h) * n : (3 + h) * n, :n]) for h in heads]
    read_val = [jnp.where(eye, own_write[h], total[(2 + h) * n : (3 + h) * n, n:]) for h in heads]

    below = row > col
    inverse = [
        jnp.where(eye, 1.0, jnp.where((differ == 1) & below, -solve_mat[h], 0.0)) for h in heads
    ]
    size = 2
    while size < n:
        level = (differ >= size) & (differ < 2 * size) & below
        inner = [dot3(jnp.where(level, solve_mat[h], 0.0), inverse[h]) for h in heads]
        inverse = [inverse[h] - dot3(inverse[h], inner[h]) for h in heads]
        size *= 2

    before = sums_of(chosen(col < row), parts)
    upto = before + log_decay
    after = sums_of(chosen(col > row), parts)
    key_start = unit * jnp.exp(before)
    read_start = recept * jnp.exp(upto)
    to_end = jnp.exp(after)
    whole = jnp.exp(upto[n - 1 : n])

    hit_val = pick_lanes([dot3(solve_val[h], value) for h in heads])
    both = jnp.concatenate([key_start, hit_val], 1)
    hits = [dot3(inverse[h], both) for h in heads]
    both = jnp.concatenate(
        [pick_lanes([hits[h][:, :c] for h in heads]), pick_lanes([hits[h][:, c:] for h in heads])],
        1,
    )
    taken = [dot3(read_rem[h], both) for h in heads]
    carried = read_start - pick_lanes([taken[h][:, :c] for h in heads])
    own_out = pick_lanes([dot3(read_val[h], value) - taken[h][:, c:] for h in heads])

    removed = dot3(removal * to_end, both, 0, 0)
    written = dot3(key * to_end, value, 0, 0)
    trans = jnp.where(eye, whole, 0.0) - removed[:, :c]
    state = written - removed[:, c:]
    pair = jnp.concatenate(
        [
            jnp.concatenate([trans[:HEAD, :HEAD], state[:HEAD, :HEAD]], 1),
            jnp.concatenate([trans[HEAD:, HEAD:], state[HEAD:, HEAD:]], 1),
        ],
        0,
    )
    return carried, own_out, pair


def compose(earlier, later):
    right = iota(later.shape, 1) >= HEAD
    return dot3(later[:, :HEAD], earlier) + jnp.where(right, later, 0.0)


class TwoPhase:
    def __init__(self, buf, send_sem, recv_sem, place, ny, nx):
        self.buf, self.send_sem, self.recv_sem = buf, send_sem, recv_sem
        self.ep, self.y, self.x = place
        self.ny, self.nx = ny, nx
        self.half = buf.shape[2] // 2

    def block(self, half, phase, step):
        rows = pl.ds(half * self.half, self.half)
        if (half + phase) % 2 == 0:
            at = lax.rem(self.x + step + self.nx, self.nx)
            if phase == 0:
                return self.buf.at[self.y, at, rows]
            return self.buf.at[:, at, rows]
        at = lax.rem(self.y + step + self.ny, self.ny)
        if phase == 0:
            return self.buf.at[at, self.x, rows]
        return self.buf.at[at, :, rows]

    def steps(self, half, phase):
        count = self.nx if (half + phase) % 2 == 0 else self.ny
        return sorted(range(1, count), key=lambda step: -min(step, count - step))

    def sent(self, half, phase, step):
        if (half + phase) % 2 == 0:
            other = self.y * self.nx + lax.rem(self.x + step, self.nx)
        else:
            other = lax.rem(self.y + step, self.ny) * self.nx + self.x
        block = self.block(half, phase, 0)
        at = (half * 2 + phase) * 4 + step
        return pltpu.make_async_remote_copy(
            src_ref=block,
            dst_ref=block,
            send_sem=self.send_sem.at[at],
            recv_sem=self.recv_sem.at[at],
            device_id={"ep": self.ep, "tp": other},
            device_id_type=MESH,
        )

    def start(self, half, phase):
        for step in self.steps(half, phase):
            self.sent(half, phase, step).start()

    def finish(self, half, phase):
        for step in reversed(self.steps(half, phase)):
            wait_for(self.block(half, phase, -step), self.recv_sem.at[(half * 2 + phase) * 4 + step])

    def begin(self):
        self.start(0, 0)
        self.start(1, 0)

    def turn(self):
        for half in range(2):
            self.finish(half, 0)
            self.start(half, 1)

    def end(self):
        self.finish(0, 1)
        self.finish(1, 1)

    def drain(self):
        for half in range(2):
            for phase in range(2):
                for step in self.steps(half, phase):
                    self.sent(half, phase, step).wait_send()


class Direct:
    def __init__(self, buf, send_sem, recv_sem, place, ny, nx):
        self.buf, self.send_sem, self.recv_sem = buf, send_sem, recv_sem
        self.ep, self.y, self.x = place
        self.ny, self.nx = ny, nx

    def begin(self):
        ny, nx = self.ny, self.nx
        own = self.buf.at[self.y * nx + self.x]

        def send(at, carry):
            to_y = lax.rem(self.y + at // nx + ny // 2, ny)
            to_x = lax.rem(self.x + lax.rem(at, nx) + nx // 2, nx)
            pltpu.make_async_remote_copy(
                src_ref=own,
                dst_ref=own,
                send_sem=self.send_sem,
                recv_sem=self.recv_sem,
                device_id={"ep": self.ep, "tp": to_y * nx + to_x},
                device_id_type=MESH,
            ).start()
            return carry

        self_at = (ny - ny // 2) * nx + (nx - nx // 2)
        lax.fori_loop(0, self_at, send, 0)
        lax.fori_loop(self_at + 1, ny * nx, send, 0)

    def others(self):
        return self.buf.at[pl.ds(0, self.ny * self.nx - 1)]

    def end(self):
        wait_for(self.others(), self.recv_sem)

    def drain(self):
        wait_for(self.others(), self.send_sem)


def step_of(at, n_ep):
    odd = lax.rem(at, 2)
    return odd * ((at + 1) // 2) + (1 - odd) * lax.rem(n_ep - at // 2, n_ep)


def wait_for(ref, sem):
    pltpu.make_async_copy(ref, ref, sem).wait()


def kernel(
    n_ep,
    n_y,
    n_x,
    group,
    *refs,
):
    hbm, refs = refs[:16], refs[16:]
    blend_out, expert_out, *refs = refs
    held, refs = refs[:14], refs[14:]
    recept_ref, key_ref, value_ref, fix_ref, fade_ref, erase_ref, speeds_ref, gain_ref = held[:8]
    merge_ref, rows_ref, scale_ref, picks_ref, share_ref, gate_up_ref = held[8:]
    (
        down_ref,
        send_buf,
        recv_buf,
        rows_all,
        hidden_all,
        back_buf,
        ret_buf,
        mixed_all,
        pair_buf,
        pair_in,
        chip_pairs,
        group_pairs,
        state_out,
        state_in,
        load_sem,
        ep_send,
        ep_recv,
        x_send,
        x_recv,
        h_send,
        h_recv,
        m_send,
        m_recv,
        scan_send,
        scan_recv,
    ) = refs
    ep, tp = lax.axis_index("ep"), lax.axis_index("tp")
    core, z = lax.rem(ep, 2), ep // 2
    y, x = tp // n_x, lax.rem(tp, n_x)
    place = lax.rem(z, group)
    n_group = n_ep // 2 // group
    mine = z // group
    partner = ep + 1 - 2 * core
    n, c = key_ref.shape
    n_rows = rows_ref.shape[0]
    lanes = send_buf.shape[2]
    slots = n_ep * SLOTS
    part = n_ep // CHUNKS
    depth = hbm[13].shape[1]

    barrier = pltpu.get_barrier_semaphore()

    def greet(step, carry):
        pl.semaphore_signal(
            barrier,
            inc=1,
            device_id={"ep": lax.rem(ep + step, n_ep), "tp": tp},
            device_id_type=MESH,
        )
        return carry

    lax.fori_loop(1, n_ep, greet, 0)

    def greet_tp(step, carry):
        pl.semaphore_signal(
            barrier,
            inc=1,
            device_id={"ep": ep, "tp": lax.rem(tp + step, n_y * n_x)},
            device_id_type=MESH,
        )
        return carry

    lax.fori_loop(1, n_y * n_x, greet_tp, 0)

    wide = [gate_up_ref.at[:, pl.ds(0, depth)], gate_up_ref.at[:, pl.ds(depth, depth)], down_ref]
    targets = [*held[:13], *wide]
    loads = [
        pltpu.make_async_copy(hbm[at], targets[at], load_sem.at[at]) for at in range(len(targets))
    ]
    order = (9, 11, 10, 12, *range(8), 13, 14, 15, 8)
    for at in order:
        loads[at].start()
    for at in order[:4]:
        loads[at].wait()

    widened = rows_ref[...].astype(F32)
    strength = lax.rsqrt(jnp.mean(widened * widened, axis=1, keepdims=True) + 1e-6)
    own = pl.ds(pl.multiple_of(tp * lanes, 128), lanes)
    normed = (rows_ref[:, own].astype(F32) * strength * scale_ref[:, own]).astype(BF16)
    slot = iota((slots, n_rows), 0)
    expert = lax.rem(step_of(slot // SLOTS, n_ep) + ep, n_ep)
    named = [picks_ref[k : k + 1, :] == expert for k in range(2)]
    either = named[0] | named[1]
    earlier = chosen(iota((n_rows, n_rows), 0) < iota((n_rows, n_rows), 1))
    rank = dot(chosen(either), earlier, 1, 0)
    taken = either & (rank == lax.rem(slot, SLOTS).astype(F32))
    weight = jnp.where(taken & named[0], share_ref[0:1, :], 0.0) + jnp.where(
        taken & named[1], share_ref[1:2, :], 0.0
    )
    send_buf[...] = dot(chosen(taken), normed, 1, 0).reshape(n_ep, SLOTS, lanes).astype(BF16)

    for at in range(8):
        loads[at].wait()
    matrices = pair_matrices(
        recept_ref[...],
        key_ref[...],
        value_ref[...],
        fix_ref[...],
        fade_ref[...],
        erase_ref[...],
        speeds_ref[...],
    )

    pl.semaphore_wait(barrier, n_ep - 1 + n_y * n_x - 1)

    def ep_copy(src, dst, at, turn, sems):
        step = step_of(at, n_ep)
        return pltpu.make_async_remote_copy(
            src_ref=src.at[at, pl.ds(0, CAP)],
            dst_ref=dst.at[at, pl.ds(0, CAP)],
            send_sem=ep_send.at[sems],
            recv_sem=ep_recv.at[sems],
            device_id={"ep": lax.rem(ep + turn * step + n_ep, n_ep), "tp": tp},
            device_id_type=MESH,
        )

    def ep_exchange(src, dst, chunk, turn, sems):
        begin, end = max(1, chunk * part), (chunk + 1) * part

        def send(at, carry):
            ep_copy(src, dst, begin + end - 1 - at, turn, sems).start()
            return carry

        lax.fori_loop(begin, end, send, 0)
        if chunk == 0:
            dst[0] = src[0]

    def ep_bytes(buf, chunk):
        begin = max(1, chunk * part)
        return buf.at[pl.ds(begin, (chunk + 1) * part - begin), pl.ds(0, CAP)]

    for chunk in reversed(range(CHUNKS)):
        ep_exchange(send_buf, recv_buf, chunk, 1, chunk)

    carried, own_out, pair = pair_results(*matrices)
    pair_buf[...] = pair

    def scan_copy(src, dst, device, at):
        return pltpu.make_async_remote_copy(
            src_ref=src,
            dst_ref=dst,
            send_sem=scan_send.at[at],
            recv_sem=scan_recv.at[at],
            device_id={"ep": device, "tp": tp},
            device_id_type=MESH,
        )

    theirs = pair_buf.at[pl.ds(pl.multiple_of(HEAD * (1 - core), HEAD), HEAD)]
    swap = scan_copy(theirs, pair_in, partner, 0)
    swap.start()
    swap.wait_recv()
    own_pair = pair_buf[pl.ds(pl.multiple_of(HEAD * core, HEAD), HEAD), :]
    other_pair = pair_in[...]
    even = core == 0
    pair_0 = jnp.where(even, own_pair, other_pair)
    pair_1 = jnp.where(even, other_pair, own_pair)
    chip_pairs[place] = compose(pair_0, pair_1)
    local = []
    for step in range(1, group):
        at = lax.rem(place + step, group)
        local.append(
            scan_copy(
                chip_pairs.at[place],
                chip_pairs.at[place],
                2 * (mine * group + at) + core,
                step,
            )
        )
        local[-1].start()
    blank = lax.rem(iota((part * SLOTS, lanes), 0), SLOTS) >= CAP
    packed, spread = iota((part * CAP, part * SLOTS), 0), iota((part * CAP, part * SLOTS), 1)
    inner = lax.rem(spread, SLOTS)
    pack = chosen((inner < CAP) & (spread // SLOTS * CAP + inner == packed))

    spot = (ep, y, x)
    size = n_y * n_x
    xs = [
        TwoPhase(rows_all.at[k], x_send.at[k], x_recv.at[k], spot, n_y, n_x) for k in range(CHUNKS)
    ]
    hs = [
        Direct(hidden_all.at[k], h_send.at[k], h_recv.at[k], spot, n_y, n_x) for k in range(CHUNKS)
    ]
    ms = Direct(mixed_all, m_send.at[0], m_recv.at[0], spot, n_y, n_x)

    def live(buf, chunk):
        block = buf[chunk * part : (chunk + 1) * part].astype(F32).reshape(part * SLOTS, lanes)
        return jnp.where(blank, 0.0, block).astype(BF16)

    def arrive(chunk):
        wait_for(ep_bytes(recv_buf, chunk), ep_recv.at[chunk])
        rows_all[chunk, y, x] = dot(pack, live(recv_buf, chunk), 1, 0).astype(BF16)

    def gate_up(chunk):
        total = jnp.zeros((part * CAP, 2 * depth), F32)
        for j in range(size):
            total = total + dot(
                rows_all[chunk, j // n_x, j % n_x],
                gate_up_ref[j * lanes : (j + 1) * lanes, :],
                1,
                0,
            )
        gated, raised = total[:, :depth], total[:, depth:]
        hidden_all[chunk, tp] = (gated / (1.0 + jnp.exp(-gated)) * raised).astype(BF16)

    def lower(chunk):
        result = jnp.zeros((part * CAP, lanes), F32)
        for j in range(size):
            result = result + dot(
                hidden_all[chunk, j], down_ref[j * depth : (j + 1) * depth, :], 1, 0
            )
        spread_out = dot(pack, result.astype(BF16), 0, 0).reshape(part, SLOTS, lanes)
        back_buf[chunk * part : (chunk + 1) * part] = spread_out.astype(BF16)
        ep_exchange(back_buf, ret_buf, chunk, -1, CHUNKS + chunk)

    arrive(0)
    xs[0].begin()
    xs[0].turn()
    for step in range(1, group):
        at = lax.rem(place - step + group, group)
        wait_for(chip_pairs.at[at], scan_recv.at[step])
    prefix = [chip_pairs[0]]
    for at in range(1, group):
        prefix.append(compose(prefix[-1], chip_pairs[at]))
    ident = jnp.where(iota((HEAD, c), 0) == iota((HEAD, c), 1), 1.0, 0.0)
    inside = ident
    for at in range(group - 1):
        inside = jnp.where(place == at + 1, prefix[at], inside)
    group_pairs[mine] = prefix[-1]

    def group_copy(step):
        return scan_copy(
            group_pairs.at[mine],
            group_pairs.at[mine],
            2 * ((mine + step) * group + place) + core,
            group + step - 1,
        )

    for step in range(1, n_group):

        @pl.when(mine + step < n_group)
        def _(step=step):
            group_copy(step).start()

    arrive(1)
    xs[1].begin()
    xs[1].turn()
    xs[0].end()
    for load in loads[13:15]:
        load.wait()
    gate_up(0)
    hs[0].begin()
    for step in range(1, n_group):

        @pl.when(mine >= step)
        def _(step=step):
            wait_for(group_pairs.at[mine - step], scan_recv.at[group + step - 1])

    state = jnp.zeros((HEAD, c), F32)
    for at in range(n_group - 1):
        state = jnp.where(at < mine, compose(state, group_pairs[at]), state)
    state_0 = compose(state, inside)
    state_1 = compose(state_0, pair_0)
    state_out[...] = jnp.where(even, state_1, state_0)
    give = scan_copy(state_out, state_in, partner, group + n_group - 1)
    give.start()
    state_own = jnp.where(even, state_0, state_1)
    xs[1].end()
    gate_up(1)
    hs[1].begin()
    give.wait_recv()
    state_other = state_in[...]
    state_a = jnp.where(even, state_own, state_other)
    state_b = jnp.where(even, state_other, state_own)
    right = iota((HEAD, c), 1) >= HEAD
    entering = jnp.concatenate(
        [
            jnp.concatenate([state_a[:, HEAD:], jnp.zeros((HEAD, HEAD), F32)], 1),
            jnp.where(right, state_b, 0.0),
        ],
        0,
    )
    out = dot3(carried, entering) + own_out
    mean = by_head(*per_head(out), (n, c)) * (1.0 / HEAD)
    centred = out - mean
    spread_of = by_head(*per_head(centred * centred), (n, c)) * (1.0 / HEAD)
    mixed = centred * lax.rsqrt(spread_of + 0.00064) * gain_ref[...]
    mixed_all[tp] = mixed.astype(BF16)
    ms.begin()
    hs[0].end()
    loads[15].wait()
    lower(0)
    hs[1].end()
    lower(1)
    ms.end()
    loads[8].wait()
    blend = jnp.zeros(blend_out.shape, F32)
    for j in range(size):
        blend = blend + dot(mixed_all[j], merge_ref[j * c : (j + 1) * c, :], 1, 0)
    blend_out[...] = blend.astype(BF16)

    for gather in (*xs, *hs, ms):
        gather.drain()
    swap.wait_send()
    give.wait_send()
    for copy in local:
        copy.wait_send()
    for step in range(1, n_group):

        @pl.when(mine + step < n_group)
        def _(step=step):
            group_copy(step).wait_send()

    for chunk in range(CHUNKS):
        wait_for(ep_bytes(send_buf, chunk), ep_send.at[chunk])
    w_hi, w_lo = split(weight)
    share = jnp.zeros(expert_out.shape, F32)
    for chunk in range(CHUNKS):
        wait_for(ep_bytes(ret_buf, chunk), ep_recv.at[CHUNKS + chunk])
        returned = live(ret_buf, chunk)
        span = slice(chunk * part * SLOTS, (chunk + 1) * part * SLOTS)
        share = share + (dot(w_hi[span], returned, 0, 0) + dot(w_lo[span], returned, 0, 0))
    expert_out[...] = share.astype(BF16)
    for chunk in range(CHUNKS):
        wait_for(ep_bytes(back_buf, chunk), ep_send.at[CHUNKS + chunk])


def body(
    n_ep,
    n_y,
    n_x,
    group,
    recept,
    key,
    value,
    fix,
    fade,
    erase,
    speeds,
    gain,
    merge,
    rows,
    scale,
    picks,
    share,
    gate,
    up,
    down,
):
    n, c = key.shape
    n_rows, width = rows.shape
    lanes = down.shape[2]
    depth = gate.shape[2]
    chunk_rows = n_ep // CHUNKS * CAP
    n_group = n_ep // 2 // group
    scans = group + n_group
    vmem, hbm = pl.BlockSpec(memory_space=pltpu.VMEM), pl.BlockSpec(memory_space=pltpu.HBM)
    small = (recept, key, value, fix, fade, erase, speeds, gain.reshape(1, c), merge, rows)
    small = (*small, scale.reshape(1, width), picks.T, share.T)
    dma = pltpu.SemaphoreType.DMA
    return pl.pallas_call(
        lambda *refs: kernel(n_ep, n_y, n_x, group, *refs),
        out_shape=(
            jax.ShapeDtypeStruct((n, merge.shape[1]), BF16),
            jax.ShapeDtypeStruct((n_rows, lanes), BF16),
        ),
        in_specs=[hbm] * 16,
        out_specs=(vmem, vmem),
        scratch_shapes=[
            *(pltpu.VMEM(array.shape, array.dtype) for array in small),
            pltpu.VMEM((width, 2 * depth), BF16),
            pltpu.VMEM(down.shape[1:], BF16),
            pltpu.VMEM((n_ep, SLOTS, lanes), BF16),
            pltpu.VMEM((n_ep, SLOTS, lanes), BF16),
            pltpu.VMEM((CHUNKS, n_y, n_x, chunk_rows, lanes), BF16),
            pltpu.VMEM((CHUNKS, n_y * n_x, chunk_rows, depth), BF16),
            pltpu.VMEM((n_ep, SLOTS, lanes), BF16),
            pltpu.VMEM((n_ep, SLOTS, lanes), BF16),
            pltpu.VMEM((n_y * n_x, n, c), BF16),
            pltpu.VMEM((n, c), F32),
            pltpu.VMEM((HEAD, c), F32),
            pltpu.VMEM((group, HEAD, c), F32),
            pltpu.VMEM((n_group, HEAD, c), F32),
            pltpu.VMEM((HEAD, c), F32),
            pltpu.VMEM((HEAD, c), F32),
            dma((16,)),
            dma((2 * CHUNKS,)),
            dma((2 * CHUNKS,)),
            dma((CHUNKS, 16)),
            dma((CHUNKS, 16)),
            dma((CHUNKS,)),
            dma((CHUNKS,)),
            dma((1,)),
            dma((1,)),
            dma((scans,)),
            dma((scans,)),
        ],
        compiler_params=pltpu.CompilerParams(
            collective_id=0, has_side_effects=True, vmem_limit_bytes=56 << 20
        ),
    )(*small, gate[0], up[0], down[0])


def solution(mesh):
    n_ep, n_tp = mesh.shape["ep"], mesh.shape["tp"]
    n_x = 4
    group = 4
    placed = (
        *(P("ep", "tp"),) * 6,
        P(None, "tp"),
        P("tp"),
        P(None, "tp"),
        P("ep", None),
        P(),
        P("ep", None),
        P("ep", None),
        *(P("ep", None, "tp"),) * 3,
    )
    return jax.shard_map(
        lambda *args: body(n_ep, n_tp // n_x, n_x, group, *args),
        mesh=mesh,
        in_specs=placed,
        out_specs=(P("ep", "tp"), P("ep", "tp")),
        check_vma=False,
    )
```

```python
import jax
import jax.numpy as jnp
from jax import lax
from jax.experimental import pallas as pl
from jax.experimental.pallas import tpu as pltpu
from jax.sharding import PartitionSpec as P

HEAD = 64
SLOTS = 8
CAP = 6
CHUNKS = 2
F32, BF16 = jnp.float32, jnp.bfloat16
MESH = pl.DeviceIdType.MESH


def dot(a, b, ca, cb):
    return lax.dot_general(a, b, (((ca,), (cb,)), ((), ())), preferred_element_type=F32)


def split(a):
    high = a.astype(BF16)
    return high, (a - high.astype(F32)).astype(BF16)


def dot3(a, b, ca=1, cb=0):
    a_hi, a_lo = split(a)
    b_hi, b_lo = split(b)
    return dot(a_hi, b_hi, ca, cb) + (dot(a_hi, b_lo, ca, cb) + dot(a_lo, b_hi, ca, cb))


def sums_of(choice, parts):
    return sum(dot(choice, part, 1, 0) for part in parts)


def chosen(mask):
    return mask.astype(F32).astype(BF16)


def iota(shape, axis):
    return lax.broadcasted_iota(jnp.int32, shape, axis)


def per_head(array):
    first = iota(array.shape, 1) < HEAD
    low = jnp.sum(jnp.where(first, array, 0.0), axis=1, keepdims=True)
    high = jnp.sum(jnp.where(first, 0.0, array), axis=1, keepdims=True)
    return low, high


def by_head(low, high, shape):
    return jnp.where(iota(shape, 1) < HEAD, low, high)


def pair_matrices(recept, key, value, fix, fade, erase, speeds):
    n, c = key.shape
    recept, key, value = recept.astype(F32), key.astype(F32), value.astype(F32)
    log_decay = -jnp.exp(speeds[0:1] + fade.astype(F32)) - erase.astype(F32)
    log_decay = jnp.maximum(log_decay, -100.0)
    learn = 1.0 / (1.0 + jnp.exp(-(fix.astype(F32) + speeds[1:2])))
    first = iota((n, c), 1) < HEAD
    unit = key * lax.rsqrt(by_head(*per_head(key * key), (n, c)) + 1e-6)
    removal = unit * learn

    part_a = log_decay.astype(BF16)
    rest = log_decay - part_a.astype(F32)
    part_b = rest.astype(BF16)
    part_c = (rest - part_b.astype(F32)).astype(BF16)
    parts = (part_a, part_b, part_c)

    row, col, pos = iota((n, n), 0), iota((n, n), 1), iota((n, c), 0)
    differ = row ^ col

    def both_heads(array):
        return jnp.concatenate([jnp.where(first, array, 0.0), jnp.where(first, 0.0, array)], 0)

    total = jnp.zeros((4 * n, 2 * n), F32)
    size = 1
    while size < n:
        later = (row & size) != 0
        mid = row & ~(size - 1)
        key_rows = chosen(later & (col >= mid) & (col < row))
        read_rows = chosen(later & (col >= mid) & (col <= row))
        end = (row | (size - 1)) + 1
        write_rows = chosen(jnp.logical_not(later) & (col > row) & (col < end))
        is_later = (pos & size) != 0
        key_in = jnp.where(is_later, unit * jnp.exp(sums_of(key_rows, parts)), 0.0)
        read_in = jnp.where(is_later, recept * jnp.exp(sums_of(read_rows, parts)), 0.0)
        fading = jnp.where(is_later, 0.0, jnp.exp(sums_of(write_rows, parts)))
        left = jnp.concatenate([both_heads(key_in), both_heads(read_in)], 0)
        right = jnp.concatenate([removal * fading, key * fading], 0)
        found = dot3(left, right, 1, 1)
        level = (differ >= size) & (differ < 2 * size) & (row > col)
        level = jnp.concatenate([level, level], 1)
        level = jnp.concatenate([level, level, level, level], 0)
        total = jnp.where(level, found, total)
        size *= 2
    return recept, key, value, unit, removal, log_decay, parts, total


def pair_results(recept, key, value, unit, removal, log_decay, parts, total):
    n, c = key.shape
    row, col = iota((n, n), 0), iota((n, n), 1)
    differ = row ^ col
    first = iota((n, c), 1) < HEAD

    def pick_lanes(pair):
        return jnp.where(first, pair[0], pair[1])

    eye = row == col
    own_write = per_head(recept * key)
    own_removal = per_head(recept * removal)
    heads = range(2)
    solve_mat = [total[h * n : (h + 1) * n, :n] for h in heads]
    solve_val = [total[h * n : (h + 1) * n, n:] for h in heads]
    read_rem = [jnp.where(eye, own_removal[h], total[(2 + h) * n : (3 + h) * n, :n]) for h in heads]
    read_val = [jnp.where(eye, own_write[h], total[(2 + h) * n : (3 + h) * n, n:]) for h in heads]

    below = row > col
    inverse = [
        jnp.where(eye, 1.0, jnp.where((differ == 1) & below, -solve_mat[h], 0.0)) for h in heads
    ]
    size = 2
    while size < n:
        level = (differ >= size) & (differ < 2 * size) & below
        inner = [dot3(jnp.where(level, solve_mat[h], 0.0), inverse[h]) for h in heads]
        inverse = [inverse[h] - dot3(inverse[h], inner[h]) for h in heads]
        size *= 2

    before = sums_of(chosen(col < row), parts)
    upto = before + log_decay
    after = sums_of(chosen(col > row), parts)
    key_start = unit * jnp.exp(before)
    read_start = recept * jnp.exp(upto)
    to_end = jnp.exp(after)
    whole = jnp.exp(upto[n - 1 : n])

    hit_val = pick_lanes([dot3(solve_val[h], value) for h in heads])
    both = jnp.concatenate([key_start, hit_val], 1)
    hits = [dot3(inverse[h], both) for h in heads]
    both = jnp.concatenate(
        [pick_lanes([hits[h][:, :c] for h in heads]), pick_lanes([hits[h][:, c:] for h in heads])],
        1,
    )
    taken = [dot3(read_rem[h], both) for h in heads]
    carried = read_start - pick_lanes([taken[h][:, :c] for h in heads])
    own_out = pick_lanes([dot3(read_val[h], value) - taken[h][:, c:] for h in heads])

    removed = dot3(removal * to_end, both, 0, 0)
    written = dot3(key * to_end, value, 0, 0)
    trans = jnp.where(eye, whole, 0.0) - removed[:, :c]
    state = written - removed[:, c:]
    pair = jnp.concatenate(
        [
            jnp.concatenate([trans[:HEAD, :HEAD], state[:HEAD, :HEAD]], 1),
            jnp.concatenate([trans[HEAD:, HEAD:], state[HEAD:, HEAD:]], 1),
        ],
        0,
    )
    return carried, own_out, pair


def compose(earlier, later):
    right = iota(later.shape, 1) >= HEAD
    return dot3(later[:, :HEAD], earlier) + jnp.where(right, later, 0.0)


class TwoPhase:
    def __init__(self, buf, send_sem, recv_sem, place, ny, nx):
        self.buf, self.send_sem, self.recv_sem = buf, send_sem, recv_sem
        self.ep, self.y, self.x = place
        self.ny, self.nx = ny, nx
        self.half = buf.shape[2] // 2

    def along_x(self, half, phase):
        return (half + phase) % 2 == 0

    def rows(self, half):
        return pl.ds(half * self.half, self.half)

    def moved(self, half, phase, step):
        if self.along_x(half, phase):
            return self.y, lax.rem(self.x + step + self.nx, self.nx)
        return lax.rem(self.y + step + self.ny, self.ny), self.x

    def steps(self, half, phase):
        count = self.nx if self.along_x(half, phase) else self.ny
        return sorted(range(1, count), key=lambda step: -min(step, count - step))

    def send(self, half, phase, block, step, out, into):
        at = self.buf.at[block[0], block[1], self.rows(half)]
        to_y, to_x = self.moved(half, phase, step)
        pltpu.make_async_remote_copy(
            src_ref=at,
            dst_ref=at,
            send_sem=self.send_sem.at[half * 2 + out],
            recv_sem=self.recv_sem.at[half * 4 + into],
            device_id={"ep": self.ep, "tp": to_y * self.nx + to_x},
            device_id_type=MESH,
        ).start()

    def begin(self):
        own = (self.y, self.x)
        for half in range(2):
            for step in self.steps(half, 0):
                self.send(half, 0, own, step, 0, step)
        for half in range(2):
            for step in self.steps(half, 1):
                self.send(half, 1, own, step, 0, 0)

    def turn(self):
        for index in range(3):
            for half in range(2):
                step = self.steps(half, 0)[2 - index]
                block = self.moved(half, 0, -step)
                at = self.buf.at[block[0], block[1], self.rows(half)]
                wait_for(at, self.recv_sem.at[half * 4 + step])
                for to in self.steps(half, 1):
                    self.send(half, 1, block, to, 1, 0)

    def blocks(self, half, count_y, count_x):
        return self.buf.at[pl.ds(0, count_y), pl.ds(0, count_x), self.rows(half)]

    def end(self):
        for half in range(2):
            wait_for(self.blocks(half, 3, 4), self.recv_sem.at[half * 4])

    def drain(self):
        for half in range(2):
            wait_for(self.blocks(half, 2, 3), self.send_sem.at[half * 2])
            wait_for(self.blocks(half, 3, 3), self.send_sem.at[half * 2 + 1])


class Direct:
    def __init__(self, buf, send_sem, recv_sem, place, ny, nx):
        self.buf, self.send_sem, self.recv_sem = buf, send_sem, recv_sem
        self.ep, self.y, self.x = place
        self.ny, self.nx = ny, nx

    def begin(self):
        ny, nx = self.ny, self.nx
        own = self.buf.at[self.y * nx + self.x]

        def send(at, carry):
            to_y = lax.rem(self.y + at // nx + ny // 2, ny)
            to_x = lax.rem(self.x + lax.rem(at, nx) + nx // 2, nx)
            pltpu.make_async_remote_copy(
                src_ref=own,
                dst_ref=own,
                send_sem=self.send_sem,
                recv_sem=self.recv_sem,
                device_id={"ep": self.ep, "tp": to_y * nx + to_x},
                device_id_type=MESH,
            ).start()
            return carry

        self_at = (ny - ny // 2) * nx + (nx - nx // 2)
        lax.fori_loop(0, self_at, send, 0)
        lax.fori_loop(self_at + 1, ny * nx, send, 0)

    def others(self):
        return self.buf.at[pl.ds(0, self.ny * self.nx - 1)]

    def end(self):
        wait_for(self.others(), self.recv_sem)

    def drain(self):
        wait_for(self.others(), self.send_sem)


def step_of(at, n_ep):
    odd = lax.rem(at, 2)
    return odd * ((at + 1) // 2) + (1 - odd) * lax.rem(n_ep - at // 2, n_ep)


def wait_for(ref, sem):
    pltpu.make_async_copy(ref, ref, sem).wait()


def kernel(
    n_ep,
    n_y,
    n_x,
    group,
    *refs,
):
    hbm, refs = refs[:16], refs[16:]
    blend_out, expert_out, *refs = refs
    held, refs = refs[:14], refs[14:]
    recept_ref, key_ref, value_ref, fix_ref, fade_ref, erase_ref, speeds_ref, gain_ref = held[:8]
    merge_ref, rows_ref, scale_ref, picks_ref, share_ref, gate_up_ref = held[8:]
    (
        down_ref,
        send_buf,
        recv_buf,
        rows_all,
        hidden_all,
        back_buf,
        ret_buf,
        mixed_all,
        pair_buf,
        pair_in,
        chip_pairs,
        group_pairs,
        state_out,
        state_in,
        load_sem,
        ep_send,
        ep_recv,
        x_send,
        x_recv,
        h_send,
        h_recv,
        m_send,
        m_recv,
        scan_send,
        scan_recv,
    ) = refs
    ep, tp = lax.axis_index("ep"), lax.axis_index("tp")
    core, z = lax.rem(ep, 2), ep // 2
    y, x = tp // n_x, lax.rem(tp, n_x)
    place = lax.rem(z, group)
    n_group = n_ep // 2 // group
    mine = z // group
    partner = ep + 1 - 2 * core
    n, c = key_ref.shape
    n_rows = rows_ref.shape[0]
    lanes = send_buf.shape[2]
    slots = n_ep * SLOTS
    part = n_ep // CHUNKS
    depth = hbm[13].shape[1]

    barrier = pltpu.get_barrier_semaphore()

    def greet(at_ep, at_tp):
        pl.semaphore_signal(
            barrier, inc=1, device_id={"ep": at_ep, "tp": at_tp}, device_id_type=MESH
        )

    for step in sorted(range(1, n_ep), key=lambda step: -min(step, n_ep - step)):
        greet(lax.rem(ep + step, n_ep), tp)
    for step in range(1, n_y * n_x):
        greet(ep, lax.rem(tp + step, n_y * n_x))

    wide = [gate_up_ref.at[:, pl.ds(0, depth)], gate_up_ref.at[:, pl.ds(depth, depth)], down_ref]
    targets = [*held[:13], *wide]
    loads = [
        pltpu.make_async_copy(hbm[at], targets[at], load_sem.at[at]) for at in range(len(targets))
    ]
    order = (9, 11, 10, 12, *range(8), 13, 14, 15, 8)
    for at in order:
        loads[at].start()
    for at in order[:4]:
        loads[at].wait()

    widened = rows_ref[...].astype(F32)
    strength = lax.rsqrt(jnp.mean(widened * widened, axis=1, keepdims=True) + 1e-6)
    own = pl.ds(pl.multiple_of(tp * lanes, 128), lanes)
    normed = (rows_ref[:, own].astype(F32) * strength * scale_ref[:, own]).astype(BF16)
    slot = iota((slots, n_rows), 0)
    expert = lax.rem(step_of(slot // SLOTS, n_ep) + ep, n_ep)
    named = [picks_ref[k : k + 1, :] == expert for k in range(2)]
    either = named[0] | named[1]
    earlier = chosen(iota((n_rows, n_rows), 0) < iota((n_rows, n_rows), 1))
    rank = dot(chosen(either), earlier, 1, 0)
    taken = either & (rank == lax.rem(slot, SLOTS).astype(F32))
    weight = jnp.where(taken & named[0], share_ref[0:1, :], 0.0) + jnp.where(
        taken & named[1], share_ref[1:2, :], 0.0
    )
    send_buf[...] = dot(chosen(taken), normed, 1, 0).reshape(n_ep, SLOTS, lanes).astype(BF16)

    for at in range(8):
        loads[at].wait()
    matrices = pair_matrices(
        recept_ref[...],
        key_ref[...],
        value_ref[...],
        fix_ref[...],
        fade_ref[...],
        erase_ref[...],
        speeds_ref[...],
    )

    pl.semaphore_wait(barrier, n_ep - 1 + n_y * n_x - 1)

    def ep_copy(src, dst, at, turn, sems):
        step = step_of(at, n_ep)
        return pltpu.make_async_remote_copy(
            src_ref=src.at[at, pl.ds(0, CAP)],
            dst_ref=dst.at[at, pl.ds(0, CAP)],
            send_sem=ep_send.at[sems],
            recv_sem=ep_recv.at[sems],
            device_id={"ep": lax.rem(ep + turn * step + n_ep, n_ep), "tp": tp},
            device_id_type=MESH,
        )

    def ep_exchange(src, dst, chunk, turn, sems):
        begin, end = max(1, chunk * part), (chunk + 1) * part

        def send(at, carry):
            ep_copy(src, dst, begin + end - 1 - at, turn, sems).start()
            return carry

        lax.fori_loop(begin, end, send, 0)
        if chunk == 0:
            dst[0] = src[0]

    def ep_bytes(buf, chunk):
        begin = max(1, chunk * part)
        return buf.at[pl.ds(begin, (chunk + 1) * part - begin), pl.ds(0, CAP)]

    for chunk in range(CHUNKS):
        ep_exchange(send_buf, recv_buf, chunk, 1, chunk)

    blank = lax.rem(iota((part * SLOTS, lanes), 0), SLOTS) >= CAP
    packed, spread = iota((part * CAP, part * SLOTS), 0), iota((part * CAP, part * SLOTS), 1)
    inner = lax.rem(spread, SLOTS)
    pack = chosen((inner < CAP) & (spread // SLOTS * CAP + inner == packed))

    spot = (ep, y, x)
    size = n_y * n_x
    xs = [
        TwoPhase(rows_all.at[k], x_send.at[k], x_recv.at[k], spot, n_y, n_x) for k in range(CHUNKS)
    ]
    hs = [
        Direct(hidden_all.at[k], h_send.at[k], h_recv.at[k], spot, n_y, n_x) for k in range(CHUNKS)
    ]
    ms = TwoPhase(mixed_all, m_send, m_recv, spot, n_y, n_x)

    def live(buf, chunk):
        block = buf[chunk * part : (chunk + 1) * part].astype(F32).reshape(part * SLOTS, lanes)
        return jnp.where(blank, 0.0, block).astype(BF16)

    def arrive(chunk):
        wait_for(ep_bytes(recv_buf, chunk), ep_recv.at[chunk])
        rows_all[chunk, y, x] = dot(pack, live(recv_buf, chunk), 1, 0).astype(BF16)

    def gate_up(chunk):
        total = jnp.zeros((part * CAP, 2 * depth), F32)
        for j in range(size):
            total = total + dot(
                rows_all[chunk, j // n_x, j % n_x],
                gate_up_ref[j * lanes : (j + 1) * lanes, :],
                1,
                0,
            )
        gated, raised = total[:, :depth], total[:, depth:]
        hidden_all[chunk, tp] = (gated / (1.0 + jnp.exp(-gated)) * raised).astype(BF16)

    def lower(chunk):
        result = jnp.zeros((part * CAP, lanes), F32)
        for j in range(0, size, 2):
            left = jnp.concatenate([hidden_all[chunk, j], hidden_all[chunk, j + 1]], 1)
            result = result + dot(left, down_ref[j * depth : (j + 2) * depth, :], 1, 0)
        spread_out = dot(pack, result.astype(BF16), 0, 0).reshape(part, SLOTS, lanes)
        back_buf[chunk * part : (chunk + 1) * part] = spread_out.astype(BF16)
        ep_exchange(back_buf, ret_buf, chunk, -1, CHUNKS + chunk)

    carried, own_out, pair = pair_results(*matrices)
    pair_buf[...] = pair

    def scan_copy(src, dst, device, at):
        return pltpu.make_async_remote_copy(
            src_ref=src,
            dst_ref=dst,
            send_sem=scan_send.at[at],
            recv_sem=scan_recv.at[at],
            device_id={"ep": device, "tp": tp},
            device_id_type=MESH,
        )

    theirs = pair_buf.at[pl.ds(pl.multiple_of(HEAD * (1 - core), HEAD), HEAD)]
    swap = scan_copy(theirs, pair_in, partner, 0)
    swap.start()
    arrive(0)
    xs[0].begin()
    swap.wait_recv()
    own_pair = pair_buf[pl.ds(pl.multiple_of(HEAD * core, HEAD), HEAD), :]
    other_pair = pair_in[...]
    even = core == 0
    pair_0 = jnp.where(even, own_pair, other_pair)
    pair_1 = jnp.where(even, other_pair, own_pair)
    chip_pairs[place] = compose(pair_0, pair_1)
    local = []
    for step in range(1, group):
        at = lax.rem(place + step, group)
        local.append(
            scan_copy(
                chip_pairs.at[place],
                chip_pairs.at[place],
                2 * (mine * group + at) + core,
                step,
            )
        )
        local[-1].start()
    xs[0].turn()
    arrive(1)
    xs[1].begin()
    for step in range(1, group):
        at = lax.rem(place - step + group, group)
        wait_for(chip_pairs.at[at], scan_recv.at[step])
    prefix = [chip_pairs[0]]
    for at in range(1, group):
        prefix.append(compose(prefix[-1], chip_pairs[at]))
    ident = jnp.where(iota((HEAD, c), 0) == iota((HEAD, c), 1), 1.0, 0.0)
    inside = ident
    for at in range(group - 1):
        inside = jnp.where(place == at + 1, prefix[at], inside)
    group_pairs[mine] = prefix[-1]

    def group_copy(step):
        return scan_copy(
            group_pairs.at[mine],
            group_pairs.at[mine],
            2 * ((mine + step) * group + place) + core,
            group + step - 1,
        )

    for step in range(1, n_group):

        @pl.when(mine + step < n_group)
        def _(step=step):
            group_copy(step).start()

    xs[1].turn()
    xs[0].end()
    for load in loads[13:15]:
        load.wait()
    gate_up(0)
    hs[0].begin()
    xs[1].end()
    gate_up(1)
    hs[1].begin()
    for step in range(1, n_group):

        @pl.when(mine >= step)
        def _(step=step):
            wait_for(group_pairs.at[mine - step], scan_recv.at[group + step - 1])

    state = jnp.zeros((HEAD, c), F32)
    for at in range(n_group - 1):
        state = jnp.where(at < mine, compose(state, group_pairs[at]), state)
    state_0 = compose(state, inside)
    state_1 = compose(state_0, pair_0)
    state_out[...] = jnp.where(even, state_1, state_0)
    give = scan_copy(state_out, state_in, partner, group + n_group - 1)
    give.start()
    state_own = jnp.where(even, state_0, state_1)
    hs[0].end()
    loads[15].wait()
    lower(0)
    give.wait_recv()
    state_other = state_in[...]
    state_a = jnp.where(even, state_own, state_other)
    state_b = jnp.where(even, state_other, state_own)
    right = iota((HEAD, c), 1) >= HEAD
    entering = jnp.concatenate(
        [
            jnp.concatenate([state_a[:, HEAD:], jnp.zeros((HEAD, HEAD), F32)], 1),
            jnp.where(right, state_b, 0.0),
        ],
        0,
    )
    out = dot3(carried, entering) + own_out
    mean = by_head(*per_head(out), (n, c)) * (1.0 / HEAD)
    centred = out - mean
    spread_of = by_head(*per_head(centred * centred), (n, c)) * (1.0 / HEAD)
    mixed = centred * lax.rsqrt(spread_of + 0.00064) * gain_ref[...]
    mixed_all[y, x] = mixed.astype(BF16)
    ms.begin()
    hs[1].end()
    lower(1)
    ms.turn()
    ms.end()
    loads[8].wait()
    blend = jnp.zeros(blend_out.shape, F32)
    for j in range(0, size, 2):
        at_y, at_x = j // n_x, j % n_x
        left = jnp.concatenate([mixed_all[at_y, at_x], mixed_all[at_y, at_x + 1]], 1)
        blend = blend + dot(left, merge_ref[j * c : (j + 2) * c, :], 1, 0)
    blend_out[...] = blend.astype(BF16)

    for gather in (*xs, *hs, ms):
        gather.drain()
    swap.wait_send()
    give.wait_send()
    for copy in local:
        copy.wait_send()
    for step in range(1, n_group):

        @pl.when(mine + step < n_group)
        def _(step=step):
            group_copy(step).wait_send()

    for chunk in range(CHUNKS):
        wait_for(ep_bytes(send_buf, chunk), ep_send.at[chunk])
    w_hi, w_lo = split(weight)
    share = jnp.zeros(expert_out.shape, F32)
    for chunk in range(CHUNKS):
        wait_for(ep_bytes(ret_buf, chunk), ep_recv.at[CHUNKS + chunk])
        returned = live(ret_buf, chunk)
        span = slice(chunk * part * SLOTS, (chunk + 1) * part * SLOTS)
        share = share + (dot(w_hi[span], returned, 0, 0) + dot(w_lo[span], returned, 0, 0))
    expert_out[...] = share.astype(BF16)
    for chunk in range(CHUNKS):
        wait_for(ep_bytes(back_buf, chunk), ep_send.at[CHUNKS + chunk])


def body(
    n_ep,
    n_y,
    n_x,
    group,
    recept,
    key,
    value,
    fix,
    fade,
    erase,
    speeds,
    gain,
    merge,
    rows,
    scale,
    picks,
    share,
    gate,
    up,
    down,
):
    n, c = key.shape
    n_rows, width = rows.shape
    lanes = down.shape[2]
    depth = gate.shape[2]
    chunk_rows = n_ep // CHUNKS * CAP
    n_group = n_ep // 2 // group
    scans = group + n_group
    vmem, hbm = pl.BlockSpec(memory_space=pltpu.VMEM), pl.BlockSpec(memory_space=pltpu.HBM)
    small = (recept, key, value, fix, fade, erase, speeds, gain.reshape(1, c), merge, rows)
    small = (*small, scale.reshape(1, width), picks.T, share.T)
    dma = pltpu.SemaphoreType.DMA
    return pl.pallas_call(
        lambda *refs: kernel(n_ep, n_y, n_x, group, *refs),
        out_shape=(
            pltpu.VMEM((n, merge.shape[1]), BF16),
            pltpu.VMEM((n_rows, lanes), BF16),
        ),
        in_specs=[hbm] * 16,
        out_specs=(vmem, vmem),
        scratch_shapes=[
            *(pltpu.VMEM(array.shape, array.dtype) for array in small),
            pltpu.VMEM((width, 2 * depth), BF16),
            pltpu.VMEM(down.shape[1:], BF16),
            pltpu.VMEM((n_ep, SLOTS, lanes), BF16),
            pltpu.VMEM((n_ep, SLOTS, lanes), BF16),
            pltpu.VMEM((CHUNKS, n_y, n_x, chunk_rows, lanes), BF16),
            pltpu.VMEM((CHUNKS, n_y * n_x, chunk_rows, depth), BF16),
            pltpu.VMEM((n_ep, SLOTS, lanes), BF16),
            pltpu.VMEM((n_ep, SLOTS, lanes), BF16),
            pltpu.VMEM((n_y, n_x, n, c), BF16),
            pltpu.VMEM((n, c), F32),
            pltpu.VMEM((HEAD, c), F32),
            pltpu.VMEM((group, HEAD, c), F32),
            pltpu.VMEM((n_group, HEAD, c), F32),
            pltpu.VMEM((HEAD, c), F32),
            pltpu.VMEM((HEAD, c), F32),
            dma((16,)),
            dma((2 * CHUNKS,)),
            dma((2 * CHUNKS,)),
            dma((CHUNKS, 4)),
            dma((CHUNKS, 8)),
            dma((CHUNKS,)),
            dma((CHUNKS,)),
            dma((4,)),
            dma((8,)),
            dma((scans,)),
            dma((scans,)),
        ],
        compiler_params=pltpu.CompilerParams(
            collective_id=0, has_side_effects=True, vmem_limit_bytes=56 << 20
        ),
    )(*small, gate[0], up[0], down[0])


def solution(mesh):
    n_ep, n_tp = mesh.shape["ep"], mesh.shape["tp"]
    n_x = 4
    group = 4
    placed = (
        *(P("ep", "tp"),) * 6,
        P(None, "tp"),
        P("tp"),
        P(None, "tp"),
        P("ep", None),
        P(),
        P("ep", None),
        P("ep", None),
        *(P("ep", None, "tp"),) * 3,
    )
    return jax.shard_map(
        lambda *args: body(n_ep, n_tp // n_x, n_x, group, *args),
        mesh=mesh,
        in_specs=placed,
        out_specs=(P("ep", "tp"), P("ep", "tp")),
        check_vma=False,
    )
```
